32 devices in a mesh: fs: 8 (over z, x), tp: 4 (over y, core).
Axes of the slice: x: 2, y: 2, z: 4, core: 2. Of those that a mesh axis runs over, the one named last changes fastest.
Arguments:
- tokens: bfloat16 [6144, 2048], P('fs', 'tp'), may hold values from -6 to 6
- mix_gain: float32 [2048], replicated, may hold values from 0.1 to 1.9
- outer_gate: bfloat16 [2048, 2048], P('fs', 'tp'), may hold values from -0.125 to 0.125
- inner_gate: bfloat16 [2048, 2048], P('fs', 'tp'), may hold values from -0.125 to 0.125
- signal_in: bfloat16 [2048, 2048], P('fs', 'tp'), may hold values from -0.125 to 0.125
- mix_taps: float32 [3, 2048], P(None, 'tp'), may hold values from -3 to 3
- mix_bias: float32 [2048], P('tp'), may hold values from -3 to 3
- mix_out: bfloat16 [2048, 2048], P('tp', 'fs'), may hold values from -0.1875 to 0.1875
- ffn_gain: float32 [2048], replicated, may hold values from 0.1 to 1.9
- up_gate: bfloat16 [2048, 5632], P('fs', 'tp'), may hold values from -0.125 to 0.125
- up_value: bfloat16 [2048, 5632], P('fs', 'tp'), may hold values from -0.125 to 0.125
- ffn_taps: float32 [2, 3, 5632], P(None, None, 'tp'), may hold values from -3 to 3
- ffn_bias: float32 [2, 5632], P(None, 'tp'), may hold values from -3 to 3
- down_proj: bfloat16 [5632, 2048], P('tp', 'fs'), may hold values from -0.109375 to 0.109375
Outputs:
- layer_out: bfloat16 [6144, 2048], P('fs', 'tp')
The draws below stay inside these ranges and needn't reach their ends.
All inputs are finite; a program needn't handle non-finite values.
Results may differ from the reference program's by a relative error of at most 0.023.
Values may be sent and summed in bfloat16 or wider, within the bound.
No kernel may reach another device: no remote copies, remote signals or barrier semaphores. Data moves between devices by JAX's collectives and lax.ppermute only.
A program may use at most 64 MiB of HBM per device.

```python
import jax
import jax.numpy as jnp
from jax import lax

D = 2048
W = 2048
FF = 5632
SEQLEN = 768
TOKENS = 6144
N_FS = 8
N_TP = 4


def with_spikes(array, key, source, target, shards_of, factor):
    owner, partner = [(jnp.arange(array.shape[position]) // (array.shape[position] // shards_of)).reshape([-1 if axis == position else 1 for axis in range(array.ndim)]) for position in (source, target)]
    chosen = jax.random.permutation(key, shards_of)[partner]
    strong = (owner == chosen) | (owner == (partner + shards_of // 2) % shards_of)
    return jnp.where(strong, factor * array, array)


def block_levels(own_key, dims, cuts, low, high):
    level, own = 1.0, jax.random.fold_in(own_key, 6)
    for dim, shards_of in cuts:
        heights = jnp.exp(jax.random.uniform(jax.random.fold_in(own, dim), (shards_of,), jnp.float32, low / len(cuts), high / len(cuts)))
        level = level * jnp.repeat(heights, dims[dim] // shards_of).reshape([-1 if axis == dim else 1 for axis in range(len(dims))])
    return level


def normal_values(own_key, shape, scale, bound, cuts=(), held_as=jnp.bfloat16):
    entries = scale * jax.random.normal(own_key, shape, jnp.float32)
    if cuts:
        entries = entries * block_levels(own_key, shape, cuts, -0.22, 0.18)
    return jnp.clip(entries, -bound, bound).astype(held_as)


def heavy_noise(rng, shape, deviation, bound, cuts, heavy, held_as=jnp.bfloat16):
    values = deviation * jax.random.normal(rng, shape, jnp.float32)
    if cuts:
        values = values * block_levels(rng, shape, cuts, -0.22, 0.18)
    return jnp.clip(with_spikes(values, jax.random.fold_in(rng, 3), *heavy), -bound, bound).astype(held_as)


def setup_inputs(seed: int = 0) -> dict:
    key_of = jax.random.split(jax.random.key(seed), 15)
    tokens = normal_values(key_of[0], (TOKENS, D), 1.0, 6.0, ((0, 8), (1, 4)))
    mix_gain = jnp.clip(1.0 + 0.18 * jax.random.normal(key_of[1], (D,), jnp.float32), 0.1, 1.9)
    outer_gate = normal_values(key_of[2], (D, W), D ** -0.5, 0.125, ((0, 8), (1, 4)))
    inner_gate = normal_values(key_of[3], (D, W), D ** -0.5, 0.125, ((0, 8), (1, 4)))
    signal_in = normal_values(key_of[4], (D, W), D ** -0.5, 0.125, ((0, 8), (1, 4)))
    mix_taps = normal_values(key_of[5], (3, W), 0.577, 3.0, ((1, 4),), jnp.float32)
    mix_bias = normal_values(key_of[6], (W,), 0.5, 3.0, ((0, 4),), jnp.float32)
    mix_out = heavy_noise(key_of[7], (W, D), W ** -0.5, 0.1875, ((0, 4), (1, 8)), (0, 1, 8, 2.0))
    ffn_gain = jnp.clip(1.0 + 0.18 * jax.random.normal(key_of[8], (D,), jnp.float32), 0.1, 1.9)
    up_gate = normal_values(key_of[9], (D, FF), D ** -0.5, 0.125, ((0, 8), (1, 4)))
    up_value = normal_values(key_of[10], (D, FF), D ** -0.5, 0.125, ((0, 8), (1, 4)))
    ffn_taps = normal_values(key_of[11], (2, 3, FF), 0.577, 3.0, ((2, 4),), jnp.float32)
    ffn_bias = normal_values(key_of[12], (2, FF), 0.5, 3.0, ((1, 4),), jnp.float32)
    down_proj = heavy_noise(key_of[13], (FF, D), FF ** -0.5, 0.109375, ((0, 4), (1, 8)), (0, 1, 8, 2.0))
    return {"tokens": tokens, "mix_gain": mix_gain, "outer_gate": outer_gate, "inner_gate": inner_gate, "signal_in": signal_in, "mix_taps": mix_taps, "mix_bias": mix_bias, "mix_out": mix_out, "ffn_gain": ffn_gain, "up_gate": up_gate, "up_value": up_value, "ffn_taps": ffn_taps, "ffn_bias": ffn_bias, "down_proj": down_proj}


EPS = 1e-06

def rms_rows(values, gain):
    floats = values.astype(jnp.float32)
    scaled = floats * lax.rsqrt(lax.optimization_barrier(jnp.mean(floats * floats, axis=-1, keepdims=True)) + EPS) * gain
    return scaled.astype(jnp.bfloat16)

def causal_taps(signal, taps, bias):
    shaped = signal.reshape(N_FS, SEQLEN, signal.shape[-1])
    first = jnp.pad(shaped, ((0, 0), (1, 0), (0, 0)))[:, :-1]
    second = jnp.pad(shaped, ((0, 0), (2, 0), (0, 0)))[:, :-2]
    result = taps[2] * shaped + taps[1] * first + taps[0] * second + bias
    return result.reshape(signal.shape)

def group_sum(active, weight):
    width = active.shape[1] // N_TP
    total = jnp.zeros((active.shape[0], weight.shape[1]), jnp.float32)
    for group in range(N_TP):
        term = jnp.dot(active[:, group * width:(group + 1) * width], weight[group * width:(group + 1) * width], preferred_element_type=jnp.float32)
        total = total + lax.optimization_barrier(term.astype(jnp.bfloat16)).astype(jnp.float32)
    return total

def reference(tokens, mix_gain, outer_gate, inner_gate, signal_in, mix_taps, mix_bias, mix_out, ffn_gain, up_gate, up_value, ffn_taps, ffn_bias, down_proj):
    normed = rms_rows(tokens, mix_gain)
    outer = jnp.dot(normed, outer_gate, preferred_element_type=jnp.float32).astype(jnp.bfloat16)
    inner = jnp.dot(normed, inner_gate, preferred_element_type=jnp.float32).astype(jnp.bfloat16)
    signal = jnp.dot(normed, signal_in, preferred_element_type=jnp.float32).astype(jnp.bfloat16)
    mixed_in = inner.astype(jnp.float32) * signal.astype(jnp.float32)
    gated = (outer.astype(jnp.float32) * causal_taps(mixed_in, mix_taps, mix_bias)).astype(jnp.bfloat16)
    mixed = group_sum(gated, mix_out)
    hidden_state = (tokens.astype(jnp.float32) + mixed).astype(jnp.bfloat16)
    normed_two = rms_rows(hidden_state, ffn_gain)
    gate_pre = jnp.dot(normed_two, up_gate, preferred_element_type=jnp.float32).astype(jnp.bfloat16)
    value_pre = jnp.dot(normed_two, up_value, preferred_element_type=jnp.float32).astype(jnp.bfloat16)
    gate_conv = causal_taps(gate_pre.astype(jnp.float32), ffn_taps[0], ffn_bias[0])
    value_conv = causal_taps(value_pre.astype(jnp.float32), ffn_taps[1], ffn_bias[1])
    active = (jax.nn.silu(gate_conv) * value_conv).astype(jnp.bfloat16)
    fed = group_sum(active, down_proj)
    return (hidden_state.astype(jnp.float32) + fed).astype(jnp.bfloat16)
```

```python
import jax
import jax.numpy as jnp
from jax import lax
from jax.sharding import PartitionSpec as P

EPS = 1e-06


def gather_rows(column_part):
    return lax.all_gather(column_part, "tp", axis=1, tiled=True)


def rms_rows(values, gain):
    floats = values.astype(jnp.float32)
    scaled = floats * lax.rsqrt(jnp.mean(floats * floats, axis=-1, keepdims=True) + EPS) * gain
    return scaled.astype(jnp.bfloat16)


def causal_taps(signal, taps, bias):
    first = jnp.pad(signal, ((1, 0), (0, 0)))[:-1]
    second = jnp.pad(signal, ((2, 0), (0, 0)))[:-2]
    return taps[2] * signal + taps[1] * first + taps[0] * second + bias


def ring_order(count):
    if count % 2:
        return list(range(count))
    return list(range(0, count, 2)) + list(range(count - 1, 0, -2))


def ring_gather(shards, axes, after=None):
    count = lax.axis_size("fs")
    order = ring_order(count)
    ahead = [(order[i], order[(i + 1) % count]) for i in range(count)]
    back = [(b, a) for a, b in ahead]
    place = [0] * count
    for i, device in enumerate(order):
        place[device] = i
    position = jnp.asarray(place, jnp.int32)[lax.axis_index("fs")]
    owners = jnp.asarray(order, jnp.int32)

    if after is not None:
        shards = lax.optimization_barrier((tuple(shards), after))[0]
    full = []

    def put(buffer, piece, axis, step, row):
        start = [jnp.int32(row), jnp.int32(0)]
        start[axis] = start[axis] + owners[(position + step) % count] * (buffer.shape[axis] // count)
        return lax.dynamic_update_slice(buffer, piece, tuple(start))

    for shard, axis in zip(shards, axes):
        shape = list(shard.shape)
        shape[axis] *= count
        full.append(put(jnp.zeros(shape, shard.dtype), shard, axis, 0, 0))
    from_back, from_ahead = list(shards), list(shards)
    whole_steps = (count - 1) // 2
    for step in range(1, whole_steps + 1):
        for k, axis in enumerate(axes):
            from_back[k] = lax.ppermute(from_back[k], "fs", ahead)
            from_ahead[k] = lax.ppermute(from_ahead[k], "fs", back)
        for k, axis in enumerate(axes):
            full[k] = put(full[k], from_back[k], axis, -step, 0)
            full[k] = put(full[k], from_ahead[k], axis, step, 0)
    if count % 2 == 0 and count > 1:
        step = whole_steps + 1
        for k, axis in enumerate(axes):
            half = shards[k].shape[0] // 2
            top = lax.ppermute(from_back[k][:half], "fs", ahead)
            bottom = lax.ppermute(from_ahead[k][half:], "fs", back)
            full[k] = put(full[k], top, axis, -step, 0)
            full[k] = put(full[k], bottom, axis, step, half)
            from_back[k] = top
    return full, from_back[-1][:1, :1]


def project_out(active, weight):
    return jnp.dot(active, weight, preferred_element_type=jnp.float32)


def share_cols(term):
    return lax.psum_scatter(
        term.astype(jnp.bfloat16), "tp", scatter_dimension=1, tiled=True
    ).astype(jnp.float32)


def fold_products(normed, pieces):
    return tuple((jnp.dot(normed, piece, preferred_element_type=jnp.float32) for piece in pieces))


def on_device(
    tokens,
    mix_gain,
    outer_gate,
    inner_gate,
    signal_in,
    mix_taps,
    mix_bias,
    mix_out,
    ffn_gain,
    up_gate,
    up_value,
    ffn_taps,
    ffn_bias,
    down_proj,
):
    (outer_gate, inner_gate, signal_in, mix_out), mark = ring_gather(
        (outer_gate, inner_gate, signal_in, mix_out), (0, 0, 0, 1)
    )
    (up_gate, up_value), mark = ring_gather((up_gate, up_value), (0, 0), mark)
    (down_proj,), mark = ring_gather((down_proj,), (1,), mark)
    full_rows = gather_rows(tokens)
    normed = rms_rows(full_rows, mix_gain)
    outer, inner, signal = fold_products(
        normed,
        (
            outer_gate,
            inner_gate,
            signal_in,
        ),
    )
    outer = outer.astype(jnp.bfloat16).astype(jnp.float32)
    inner = inner.astype(jnp.bfloat16).astype(jnp.float32)
    signal = signal.astype(jnp.bfloat16).astype(jnp.float32)
    gated = (outer * causal_taps(inner * signal, mix_taps, mix_bias)).astype(jnp.bfloat16)
    mix_term = project_out(gated, mix_out)
    total = lax.psum(mix_term.astype(jnp.bfloat16), "tp").astype(jnp.float32)
    state_rows = (full_rows.astype(jnp.float32) + total).astype(jnp.bfloat16)
    own_width = tokens.shape[1]
    state_cols = lax.dynamic_slice_in_dim(
        state_rows, lax.axis_index("tp") * own_width, own_width, 1
    )
    normed_two = rms_rows(state_rows, ffn_gain)
    gate_pre, value_pre = fold_products(
        normed_two,
        (
            up_gate,
            up_value,
        ),
    )
    gate_pre = gate_pre.astype(jnp.bfloat16).astype(jnp.float32)
    value_pre = value_pre.astype(jnp.bfloat16).astype(jnp.float32)
    gate_conv = causal_taps(gate_pre, ffn_taps[0], ffn_bias[0])
    value_conv = causal_taps(value_pre, ffn_taps[1], ffn_bias[1])
    active = (jax.nn.silu(gate_conv) * value_conv).astype(jnp.bfloat16)
    fed = share_cols(project_out(active, down_proj))
    return (state_cols.astype(jnp.float32) + fed).astype(jnp.bfloat16)


def solution(mesh):
    return jax.shard_map(
        on_device,
        mesh=mesh,
        in_specs=(
            P("fs", "tp"),
            P(),
            P("fs", "tp"),
            P("fs", "tp"),
            P("fs", "tp"),
            P(None, "tp"),
            P("tp"),
            P("tp", "fs"),
            P(),
            P("fs", "tp"),
            P("fs", "tp"),
            P(None, None, "tp"),
            P(None, "tp"),
            P("tp", "fs"),
        ),
        out_specs=P("fs", "tp"),
        check_vma=False,
    )
```
